32 devices in a mesh: fs: 16 (over z, y, x), tp: 2 (over core).
Axes of the slice: x: 2, y: 2, z: 4, core: 2. Of those that a mesh axis runs over, the one named last changes fastest.
Arguments:
- inputs: bfloat16 [8192, 2048], P('fs', 'tp'), may hold values from -6 to 6
- hidden_pre: bfloat16 [8192, 4096], P('fs', 'tp'), may hold values from -6 to 6
- norm_input: bfloat16 [8192, 2048], P('fs', 'tp'), may hold values from -48 to 48, as said below
- out_gain: float32 [2048], P('tp'), may hold values from 0.1 to 1.9
- w_up: bfloat16 [2048, 4096], P('tp', 'fs'), may hold values from -0.125 to 0.125
- w_down: bfloat16 [4096, 2048], P('tp', 'fs'), may hold values from -0.09375 to 0.09375
- cotangent: bfloat16 [8192, 2048], P('fs', 'tp'), may hold values from -6 to 6
Outputs:
- grad_input: bfloat16 [8192, 2048], P('fs', 'tp')
- grad_up: float32 [2048, 4096], P('tp', 'fs')
- grad_gain: float32 [2048], P('tp')
The draws below stay inside these ranges and needn't reach their ends.
Inputs may be any that keep to these rules, and one draw needn't show every extreme that they name: `norm_input`: each token's features are scaled by a factor of that token, and each block of 2048 / 2 features by a factor of that block.
All inputs are finite; a program needn't handle non-finite values.
Results may differ from the reference program's by a relative error of at most 0.0058.
Values may be sent and summed in bfloat16 or wider, within the bound.
A program may use at most 64 MiB of HBM per device.

```python
import jax
import jax.numpy as jnp
from jax import lax

D = 2048
FF = 4096
TOKENS = 8192
N_TP = 2


def draw_norm_input(key, part):
    key_base, key_block, key_row, key_common = jax.random.split(key, 4)
    base = jnp.clip(jax.random.normal(key_base, (TOKENS, D), jnp.float32), -6.0, 6.0)
    blocks = jnp.exp(jax.random.uniform(key_block, (N_TP,), jnp.float32, -1.2, 1.2))
    columns = jnp.repeat(blocks, D // N_TP)
    rowwise = jnp.exp(jax.random.uniform(key_row, (TOKENS, 1), jnp.float32, -0.7, 0.7))
    return (base * rowwise * columns[None, :]).astype(jnp.bfloat16)


def raised(entries, key, source, target, shards_of, factor):
    def block_of(dim):
        return (jnp.arange(entries.shape[dim]) // (entries.shape[dim] // shards_of)).reshape((-1,) + (1,) * (entries.ndim - 1 - dim))

    one_side = jax.random.permutation(key, shards_of)[block_of(target)]
    other_side = (block_of(target) + shards_of // 2) % shards_of
    return jnp.where((block_of(source) == one_side) | (block_of(source) == other_side), factor * entries, entries)


def block_scale(rng, dims, pieces, least, largest):
    factor_of = 1.0
    for position, blocks in pieces:
        draws = jax.random.uniform(jax.random.fold_in(jax.random.fold_in(rng, 6), position), (blocks,), jnp.float32, least / len(pieces), largest / len(pieces))
        factor_of = factor_of * jnp.repeat(jnp.exp(draws), dims[position] // blocks).reshape((-1,) + (1,) * (len(dims) - 1 - position))
    return factor_of


def normal_values(key, dims, deviation, limit, pieces=(), dtype=jnp.bfloat16):
    level = block_scale(key, dims, pieces, -0.22, 0.18) if pieces else 1.0
    entries = jax.random.normal(key, dims, jnp.float32) * deviation * level
    return jnp.minimum(jnp.maximum(entries, -limit), limit).astype(dtype)


def noise_with(own_key, dims, width, bound, cuts, heavy, held_as=jnp.bfloat16):
    result = width * jax.random.normal(own_key, dims, jnp.float32)
    if cuts:
        result = result * block_scale(own_key, dims, cuts, -0.22, 0.18)
    return jnp.clip(raised(result, jax.random.fold_in(own_key, 3), *heavy), -bound, bound).astype(held_as)


def setup_inputs(seed: int = 0) -> dict:
    arg_keys = jax.random.split(jax.random.key(seed), 8)
    inputs = normal_values(arg_keys[0], (TOKENS, D), 1.0, 6.0, ((0, 16), (1, 2)))
    hidden_pre = normal_values(arg_keys[1], (TOKENS, FF), 1.0, 6.0, ((0, 16), (1, 2)))
    norm_input = draw_norm_input(jax.random.fold_in(arg_keys[7], 71), 0)
    out_gain = jnp.clip(1.0 + 0.18 * jax.random.normal(arg_keys[3], (D,), jnp.float32), 0.1, 1.9)
    w_up = normal_values(arg_keys[4], (D, FF), D ** -0.5, 0.125, ((0, 2), (1, 16)))
    w_down = normal_values(arg_keys[5], (FF, D), FF ** -0.5, 0.09375, ((0, 2), (1, 16)))
    cotangent = noise_with(arg_keys[6], (TOKENS, D), 1.0, 6.0, ((0, 16), (1, 2)), (0, 1, 16, 2.0))
    return dict(inputs=inputs, hidden_pre=hidden_pre, norm_input=norm_input, out_gain=out_gain, w_up=w_up, w_down=w_down, cotangent=cotangent)


norm_eps = 1e-06

def reference(inputs, hidden_pre, norm_input, out_gain, w_up, w_down, cotangent):
    scaled = TOKENS ** (-0.5)
    normed = norm_input.astype(jnp.float32)
    upstream = cotangent.astype(jnp.float32)
    inv_rms = lax.rsqrt(lax.optimization_barrier(jnp.mean(normed * normed, axis=1, keepdims=True)) + norm_eps)
    cross_mean = lax.optimization_barrier(jnp.mean(upstream * out_gain * normed, axis=1, keepdims=True))
    d_out = (upstream * out_gain * inv_rms - normed * inv_rms * inv_rms * inv_rms * cross_mean).astype(jnp.bfloat16)
    grad_gain = lax.optimization_barrier(jnp.sum(upstream * normed * inv_rms, axis=0)) * scaled
    d_act = jnp.dot(d_out, w_down.T, preferred_element_type=jnp.float32)
    d_pre = (d_act * 2.0 * jax.nn.relu(hidden_pre.astype(jnp.float32))).astype(jnp.bfloat16)
    grad_input = jnp.dot(d_pre, w_up.T, preferred_element_type=jnp.float32).astype(jnp.bfloat16)
    grad_up = jnp.dot(inputs.T, d_pre, preferred_element_type=jnp.float32) * scaled
    return (grad_input, grad_up, grad_gain)
```

```python
import jax
import jax.numpy as jnp
from jax import lax
from jax.sharding import PartitionSpec as P

norm_eps = 1e-06


def trade(x, axis, mask):
    if mask == 0:
        return x
    return lax.ppermute(x, axis, [(i, i ^ mask) for i in range(lax.axis_size(axis))])


def total(x, axis):
    step = 1
    while step < lax.axis_size(axis):
        x = x + trade(x, axis, step)
        step *= 2
    return x


def pick(stack, index):
    return lax.dynamic_index_in_dim(stack, index, 0, keepdims=False)


def dot(a, b, dim):
    return lax.dot_general(
        a, b, (((dim,), (dim,)), ((), ())), preferred_element_type=jnp.float32
    )


def on_device(inputs, hidden_pre, norm_input, out_gain, w_up, w_down, cotangent):
    fs, tp = lax.axis_size("fs"), lax.axis_size("tp")
    near_n = 1
    while 4 * near_n * near_n <= fs:
        near_n *= 2
    far_n = fs // near_n
    per = far_n // tp
    me, core = lax.axis_index("fs"), lax.axis_index("tp")
    far, near = me // near_n, me % near_n
    rows = inputs.shape[0]
    width = inputs.shape[1] * tp
    scaled = (rows * fs) ** (-0.5)
    block = w_up.shape[1]
    cols = w_down.shape[1]

    down_rows = w_down.reshape(per, near_n, block, cols)
    arrived = jnp.stack(
        [
            trade(
                lax.dynamic_index_in_dim(down_rows, near ^ k, 1, keepdims=False).reshape(
                    per * block, cols
                ),
                "fs",
                k,
            )
            for k in range(near_n)
        ]
    )
    down_near = jnp.concatenate([pick(arrived, near ^ i) for i in range(near_n)], axis=1)
    down_far = jnp.stack([trade(down_near, "fs", k * near_n) for k in range(far_n)])
    up_far = jnp.stack([trade(w_up, "fs", k * near_n) for k in range(far_n)])
    down, up = [], []
    for t in range(tp):
        places = [((core ^ t) * per + j) ^ far for j in range(per)]
        down.append(jnp.concatenate([pick(down_far, i) for i in places], axis=1))
        up.append(jnp.concatenate([pick(up_far, i) for i in places], axis=1))

    pre = [
        trade(
            jnp.concatenate(
                [
                    lax.dynamic_slice_in_dim(
                        hidden_pre, (j * near_n + (near ^ k)) * block, block, axis=1
                    )
                    for j in range(per)
                ],
                axis=1,
            ),
            "fs",
            k,
        )
        for k in range(near_n)
    ]

    normed = norm_input.astype(jnp.float32)
    upstream = cotangent.astype(jnp.float32)
    weighted = upstream * out_gain
    sums = total(
        jnp.stack([jnp.sum(normed * normed, axis=1), jnp.sum(weighted * normed, axis=1)]), "tp"
    )
    inv_rms = lax.rsqrt(sums[0] / width + norm_eps)[:, None]
    cross_mean = (sums[1] / width)[:, None]
    d_out = (weighted * inv_rms - normed * inv_rms * inv_rms * inv_rms * cross_mean).astype(
        jnp.bfloat16
    )
    grad_gain = total(jnp.sum(upstream * normed * inv_rms, axis=0) * scaled, "fs")

    d_outs = [trade(d_out, "fs", k) for k in range(near_n)]
    tokens = [trade(inputs, "fs", k) for k in range(near_n)]
    d_pres, partial = [], []
    for k in range(near_n):
        d_act = sum(dot(trade(d_outs[k], "tp", t), down[t], 1) for t in range(tp))
        d_pre = (d_act * 2.0 * jax.nn.relu(pre[k].astype(jnp.float32))).astype(jnp.bfloat16)
        d_pres.append([trade(d_pre, "tp", t) for t in range(tp)])
        partial.append(sum(dot(d_pres[k][t], up[t], 1) for t in range(tp)))
    grad_input = partial[0]
    for k in range(1, near_n):
        grad_input = grad_input + trade(partial[k].astype(jnp.bfloat16), "fs", k).astype(
            jnp.float32
        )

    all_tokens = jnp.concatenate(tokens, axis=0)
    sums_up = jnp.concatenate(
        [
            dot(jnp.concatenate([d_pres[k][t] for k in range(near_n)], axis=0), all_tokens, 0)
            for t in range(tp)
        ],
        axis=0,
    ).reshape(far_n, block, inputs.shape[1])
    grad_up = 0.0
    for k in range(far_n):
        goal = far ^ k
        mine = pick(sums_up, (core ^ (goal // per)) * per + goal % per)
        if k:
            mine = trade(mine.astype(jnp.bfloat16), "fs", k * near_n).astype(jnp.float32)
        grad_up = grad_up + mine
    return (grad_input.astype(jnp.bfloat16), (grad_up * scaled).T, grad_gain)


def solution(mesh):
    placed = (
        P("fs", "tp"),
        P("fs", "tp"),
        P("fs", "tp"),
        P("tp"),
        P("tp", "fs"),
        P("tp", "fs"),
        P("fs", "tp"),
    )
    return jax.shard_map(
        on_device,
        mesh=mesh,
        in_specs=placed,
        out_specs=(P("fs", "tp"), P("tp", "fs"), P("tp")),
        check_vma=False,
    )
```

```python
import jax
import jax.numpy as jnp
from jax import lax
from jax.sharding import PartitionSpec as P

norm_eps = 1e-06


def trade(x, axis, mask):
    if mask == 0:
        return x
    return lax.ppermute(x, axis, [(i, i ^ mask) for i in range(lax.axis_size(axis))])


def total(x, axis):
    step = 1
    while step < lax.axis_size(axis):
        x = x + trade(x, axis, step)
        step *= 2
    return x


def after(x, *others):
    return lax.optimization_barrier((x,) + others)[0]


def masks_of(n):
    masks = [1 << i for i in range(n.bit_length() - 1)]
    return (masks, masks[::-1])


def halves(x):
    rows = x.shape[0] // 2
    return (x[:rows], x[rows:])


def gather_near(x, near_n):
    parts = []
    for part, masks in zip(halves(x), masks_of(near_n)):
        held = {0: part}
        for mask in masks:
            held.update({k ^ mask: trade(v, "fs", mask) for k, v in list(held.items())})
        parts.append(held)
    return parts


def scatter_near(pieces, near_n):
    sums = []
    for side, masks in enumerate(masks_of(near_n)):
        held = {k: halves(v)[side] for k, v in pieces.items()}
        for mask in masks:
            sent = {k: held.pop(k) for k in list(held) if k & mask}
            for k, v in sent.items():
                came = trade(v.astype(jnp.bfloat16), "fs", mask).astype(jnp.float32)
                held[k ^ mask] = held[k ^ mask] + came
        sums.append(held[0])
    return jnp.concatenate(sums, axis=0)


def tree(x, n, unit):
    terms = [trade(x, "fs", k * unit) for k in range(n)]
    while len(terms) > 1:
        terms = [a + b for a, b in zip(terms[::2], terms[1::2])]
    return terms[0]


def pick(stack, index):
    return lax.dynamic_index_in_dim(stack, index, 0, keepdims=False)


def dot(a, b, dim):
    return lax.dot_general(
        a, b, (((dim,), (dim,)), ((), ())), preferred_element_type=jnp.float32
    )


def on_device(inputs, hidden_pre, norm_input, out_gain, w_up, w_down, cotangent):
    fs, tp = lax.axis_size("fs"), lax.axis_size("tp")
    near_n = 1
    while 4 * near_n * near_n <= fs:
        near_n *= 2
    far_n = fs // near_n
    per = far_n // tp
    me, core = lax.axis_index("fs"), lax.axis_index("tp")
    far, near = me // near_n, me % near_n
    rows = inputs.shape[0]
    width = inputs.shape[1] * tp
    scaled = (rows * fs) ** (-0.5)
    block = w_up.shape[1]
    cols = w_down.shape[1]

    down_rows = w_down.reshape(per, near_n, block, cols)
    arrived = jnp.stack(
        [
            trade(
                lax.dynamic_index_in_dim(down_rows, near ^ k, 1, keepdims=False).reshape(
                    per * block, cols
                ),
                "fs",
                k,
            )
            for k in range(near_n)
        ]
    )
    down_near = jnp.concatenate([pick(arrived, near ^ i) for i in range(near_n)], axis=1)
    down_far = [trade(down_near, "fs", k * near_n) for k in range(far_n)]
    w_up = after(w_up, down_far[1])
    up_far = jnp.stack([trade(w_up, "fs", k * near_n) for k in range(far_n)])
    down_far = jnp.stack(down_far)
    down, up = [], []
    for t in range(tp):
        places = [((core ^ t) * per + j) ^ far for j in range(per)]
        down.append(jnp.concatenate([pick(down_far, i) for i in places], axis=1))
        up.append(jnp.concatenate([pick(up_far, i) for i in places], axis=1))

    pre = [
        trade(
            jnp.concatenate(
                [
                    lax.dynamic_slice_in_dim(
                        hidden_pre, (j * near_n + (near ^ k)) * block, block, axis=1
                    )
                    for j in range(per)
                ],
                axis=1,
            ),
            "fs",
            k,
        )
        for k in range(near_n)
    ]

    normed = norm_input.astype(jnp.float32)
    upstream = cotangent.astype(jnp.float32)
    weighted = upstream * out_gain
    sums = total(
        jnp.stack([jnp.sum(normed * normed, axis=1), jnp.sum(weighted * normed, axis=1)]), "tp"
    )
    inv_rms = lax.rsqrt(sums[0] / width + norm_eps)[:, None]
    cross_mean = (sums[1] / width)[:, None]
    d_out = (weighted * inv_rms - normed * inv_rms * inv_rms * inv_rms * cross_mean).astype(
        jnp.bfloat16
    )
    gain_near = tree(jnp.sum(upstream * normed * inv_rms, axis=0) * scaled, near_n, 1)
    grad_gain = tree(gain_near, far_n, near_n)

    d_outs = gather_near(d_out, near_n)
    first, last = inputs.shape[1] // 2, near_n - 1
    left = after(inputs[:, :first], d_outs[0][1], gain_near)
    right = after(inputs[:, first:], d_outs[0][last], d_outs[1][last])
    tokens = [gather_near(left, near_n), gather_near(right, near_n)]
    d_pres, partial = [], {}
    for k in range(near_n):
        d_out_k = jnp.concatenate([d_outs[0][k], d_outs[1][k]], axis=0)
        d_act = sum(dot(trade(d_out_k, "tp", t), down[t], 1) for t in range(tp))
        d_pre = (d_act * 2.0 * jax.nn.relu(pre[k].astype(jnp.float32))).astype(jnp.bfloat16)
        d_pres.append([trade(d_pre, "tp", t) for t in range(tp)])
        partial[k] = sum(dot(d_pres[k][t], up[t], 1) for t in range(tp))
    grad_input = scatter_near(partial, near_n)

    all_pres = [
        jnp.concatenate([d_pres[k][t] for k in range(near_n)], axis=0) for t in range(tp)
    ]
    all_pres[0], grad_gain = lax.optimization_barrier((all_pres[0], grad_gain))
    grads = []
    for part in tokens:
        all_tokens = jnp.concatenate(
            [side[k] for k in range(near_n) for side in part], axis=0
        )
        sums_up = jnp.concatenate([dot(x, all_tokens, 0) for x in all_pres], axis=0).reshape(
            far_n, block, all_tokens.shape[1]
        )
        grad_up = 0.0
        for k in range(far_n):
            goal = far ^ k
            mine = pick(sums_up, (core ^ (goal // per)) * per + goal % per)
            if k:
                mine = trade(mine.astype(jnp.bfloat16), "fs", k * near_n).astype(jnp.float32)
            grad_up = grad_up + mine
        grads.append((grad_up * scaled).T)
    return (grad_input.astype(jnp.bfloat16), jnp.concatenate(grads, axis=0), grad_gain)


def solution(mesh):
    placed = (
        P("fs", "tp"),
        P("fs", "tp"),
        P("fs", "tp"),
        P("tp"),
        P("tp", "fs"),
        P("tp", "fs"),
        P("fs", "tp"),
    )
    return jax.shard_map(
        on_device,
        mesh=mesh,
        in_specs=placed,
        out_specs=(P("fs", "tp"), P("tp", "fs"), P("tp")),
        check_vma=False,
    )
```

```python
import jax
import jax.numpy as jnp
from jax import lax
from jax.sharding import PartitionSpec as P


norm_eps = 1e-06


def trade(x, axis, mask):
    if mask == 0:
        return x
    return lax.ppermute(x, axis, [(i, i ^ mask) for i in range(lax.axis_size(axis))])


def total(x, axis):
    step = 1
    while step < lax.axis_size(axis):
        x = x + trade(x, axis, step)
        step *= 2
    return x


def masks_of(n):
    masks = [1 << i for i in range(n.bit_length() - 1)]
    return (masks, masks[::-1])


def halves(x):
    rows = x.shape[0] // 2
    return (x[:rows], x[rows:])


def gather_near(x, near_n):
    parts = []
    for part, masks in zip(halves(x), masks_of(near_n)):
        held = {0: part}
        for mask in masks:
            held.update({k ^ mask: trade(v, "fs", mask) for k, v in list(held.items())})
        parts.append(held)
    return parts


def scatter_near(pieces, near_n):
    sums = []
    for side, masks in enumerate(masks_of(near_n)):
        held = {k: halves(v)[side] for k, v in pieces.items()}
        for mask in masks:
            sent = {k: held.pop(k) for k in list(held) if k & mask}
            for k, v in sent.items():
                came = trade(v.astype(jnp.bfloat16), "fs", mask).astype(jnp.float32)
                held[k ^ mask] = held[k ^ mask] + came
        sums.append(held[0])
    return jnp.concatenate(sums, axis=0)


def tree(x, n, unit):
    terms = [trade(x, "fs", k * unit) for k in range(n)]
    while len(terms) > 1:
        terms = [a + b for a, b in zip(terms[::2], terms[1::2])]
    return terms[0]


def pick(stack, index):
    return lax.dynamic_index_in_dim(stack, index, 0, keepdims=False)


def dot(a, b, dim):
    return lax.dot_general(
        a, b, (((dim,), (dim,)), ((), ())), preferred_element_type=jnp.float32
    )


def on_device(inputs, hidden_pre, norm_input, out_gain, w_up, w_down, cotangent):
    fs, tp = lax.axis_size("fs"), lax.axis_size("tp")
    near_n = 1
    while 4 * near_n * near_n <= fs:
        near_n *= 2
    far_n = fs // near_n
    per = far_n // tp
    me, core = lax.axis_index("fs"), lax.axis_index("tp")
    far, near = me // near_n, me % near_n
    rows = inputs.shape[0]
    width = inputs.shape[1] * tp
    scaled = (rows * fs) ** (-0.5)
    block = w_up.shape[1]
    cols = w_down.shape[1]

    down_rows = w_down.reshape(per, near_n, block, cols)
    asked = [
        lax.dynamic_index_in_dim(down_rows, near ^ k, 1, keepdims=False).reshape(per * block, cols)
        for k in range(near_n)
    ]
    arrived = [trade(x, "fs", k) for k, x in enumerate(asked)]
    arrived = jnp.stack(arrived)
    down_near = jnp.concatenate([pick(arrived, near ^ i) for i in range(near_n)], axis=1)
    down_far = [trade(down_near, "fs", k * near_n) for k in range(far_n)]
    up_far = [trade(w_up, "fs", k * near_n) for k in range(far_n)]
    up_far = jnp.stack(up_far)
    down_far = jnp.stack(down_far)
    down, up = [], []
    for t in range(tp):
        places = [((core ^ t) * per + j) ^ far for j in range(per)]
        down.append(jnp.concatenate([pick(down_far, i) for i in places], axis=1))
        up.append(jnp.concatenate([pick(up_far, i) for i in places], axis=1))

    asked = [
        jnp.concatenate(
            [
                lax.dynamic_slice_in_dim(
                    hidden_pre, (j * near_n + (near ^ k)) * block, block, axis=1
                )
                for j in range(per)
            ],
            axis=1,
        )
        for k in range(near_n)
    ]
    pre = [trade(x, "fs", k) for k, x in enumerate(asked)]

    normed = norm_input.astype(jnp.float32)
    upstream = cotangent.astype(jnp.float32)
    weighted = upstream * out_gain
    sums = total(
        jnp.stack([jnp.sum(normed * normed, axis=1), jnp.sum(weighted * normed, axis=1)]), "tp"
    )
    inv_rms = lax.rsqrt(sums[0] / width + norm_eps)[:, None]
    cross_mean = (sums[1] / width)[:, None]
    d_out = (weighted * inv_rms - normed * inv_rms * inv_rms * inv_rms * cross_mean).astype(
        jnp.bfloat16
    )
    gain = jnp.sum(upstream * normed * inv_rms, axis=0) * scaled
    gain = tree(gain, near_n, 1)
    grad_gain = tree(gain, far_n, near_n)

    d_outs = gather_near(d_out, near_n)
    tokens = gather_near(inputs, near_n)
    d_pres, partial = [], {}
    for k in range(near_n):
        d_out_k = jnp.concatenate([d_outs[0][k], d_outs[1][k]], axis=0)
        d_out_k = [trade(d_out_k, "tp", t) for t in range(tp)]
        d_act = sum(dot(d_out_k[t], down[t], 1) for t in range(tp))
        d_pre = (d_act * 2.0 * jax.nn.relu(pre[k].astype(jnp.float32))).astype(jnp.bfloat16)
        d_pres.append([trade(d_pre, "tp", t) for t in range(tp)])
        partial[k] = sum(dot(d_pres[k][t], up[t], 1) for t in range(tp))
    grad_input = scatter_near(partial, near_n)

    all_pres = [
        jnp.concatenate([d_pres[k][t] for k in range(near_n)], axis=0) for t in range(tp)
    ]
    all_tokens = jnp.concatenate([side[k] for k in range(near_n) for side in tokens], axis=0)
    sums_up = [dot(x, all_tokens, 0) for x in all_pres]
    sums_up = jnp.concatenate(sums_up, axis=0).reshape(
        far_n, block, inputs.shape[1]
    )
    grad_up = 0.0
    for k in range(far_n):
        goal = far ^ k
        mine = pick(sums_up, (core ^ (goal // per)) * per + goal % per)
        if k:
            mine = trade(mine.astype(jnp.bfloat16), "fs", k * near_n).astype(jnp.float32)
        grad_up = grad_up + mine
    return (grad_input.astype(jnp.bfloat16), (grad_up * scaled).T, grad_gain)


def solution(mesh):
    placed = (
        P("fs", "tp"),
        P("fs", "tp"),
        P("fs", "tp"),
        P("tp"),
        P("tp", "fs"),
        P("tp", "fs"),
        P("fs", "tp"),
    )
    return jax.shard_map(
        on_device,
        mesh=mesh,
        in_specs=placed,
        out_specs=(P("fs", "tp"), P("tp", "fs"), P("tp")),
        check_vma=False,
    )
```
